32 devices in a mesh: fs: 8 (over z, core), tp: 4 (over y, x).
Axes of the slice: x: 2, y: 2, z: 4, core: 2. Of those that a mesh axis runs over, the one named last changes fastest.
Arguments:
- tokens: bfloat16 [4096, 2048], P('fs'), may hold values from -6 to 6
- cotangent: bfloat16 [4096, 2048], P('fs'), may hold values from -6 to 6
- gate_weight: bfloat16 [2048, 2816], P('fs', 'tp'), may hold values from -0.125 to 0.125
- up_weight: bfloat16 [2048, 2816], P('fs', 'tp'), may hold values from -0.125 to 0.125
- down_weight: bfloat16 [2048, 2816], P('fs', 'tp'), may hold values from -0.109375 to 0.109375
Outputs:
- input_grad: bfloat16 [4096, 2048], P('fs', 'tp')
- gate_grad: float32 [2048, 2816], P('fs', 'tp')
- up_grad: float32 [2048, 2816], P('fs', 'tp')
- down_grad: float32 [2048, 2816], P('fs', 'tp')
The draws below stay inside these ranges and needn't reach their ends.
All inputs are finite; a program needn't handle non-finite values.
Results may differ from the reference program's by a relative error of at most 0.014.
Values may be sent and summed in bfloat16 or wider, within the bound.
No kernel may reach another device: no remote copies, remote signals or barrier semaphores. Data moves between devices by JAX's collectives and lax.ppermute only.
A program may use at most 64 MiB of HBM per device.

```python
import jax
import jax.numpy as jnp
from jax import lax

D = 2048
FF = 2816
TOKENS = 4096
N_TP = 4


def with_spikes(array, own_key, source, target, shards_of, factor):
    owner, partner = [(jnp.arange(array.shape[position]) // (array.shape[position] // shards_of)).reshape([-1 if axis == position else 1 for axis in range(array.ndim)]) for position in (source, target)]
    chosen = jax.random.permutation(own_key, shards_of)[partner]
    strong = (owner == chosen) | (owner == (partner + shards_of // 2) % shards_of)
    return jnp.where(strong, factor * array, array)


def block_levels(stream_key, dims, split, smallest, high):
    def one(position, shards_of):
        draws = jax.random.uniform(jax.random.fold_in(jax.random.fold_in(stream_key, 6), position), (shards_of,), jnp.float32, smallest / len(split), high / len(split))
        return jnp.repeat(jnp.exp(draws), dims[position] // shards_of).reshape((-1,) + (1,) * (len(dims) - position - 1))

    gain = one(*split[0])
    for cut in split[1:]:
        gain = gain * one(*cut)
    return gain


def centred(stream_key, extent, scale, limit, pieces=(), kind=jnp.bfloat16):
    values = jax.random.normal(stream_key, extent, jnp.float32) * scale
    if len(pieces) > 0:
        values = block_levels(stream_key, extent, pieces, -0.22, 0.18) * values
    return jnp.clip(values, min=-limit, max=limit).astype(kind)


def heavy_noise(stream_key, dims, scale, most, pieces, heavy, kind=jnp.bfloat16):
    drawn = scale * jax.random.normal(stream_key, dims, jnp.float32)
    if pieces:
        drawn = drawn * block_levels(stream_key, dims, pieces, -0.22, 0.18)
    return jnp.clip(with_spikes(drawn, jax.random.fold_in(stream_key, 3), *heavy), -most, most).astype(kind)


def setup_inputs(seed: int = 0) -> dict:
    streams_of = jax.random.split(jax.random.key(seed), 6)
    tokens = centred(streams_of[0], (TOKENS, D), 1.0, 6.0, ((0, 8),))
    cotangent = heavy_noise(streams_of[1], (TOKENS, D), 1.0, 6.0, ((0, 8),), (0, 1, 8, 2.0))
    gate_weight = centred(streams_of[2], (D, FF), D ** -0.5, 0.125, ((0, 8), (1, 4)))
    up_weight = centred(streams_of[3], (D, FF), D ** -0.5, 0.125, ((0, 8), (1, 4)))
    down_weight = centred(streams_of[4], (D, FF), FF ** -0.5, 0.109375, ((0, 8), (1, 4)))
    return dict(tokens=tokens, cotangent=cotangent, gate_weight=gate_weight, up_weight=up_weight, down_weight=down_weight)


def reference(tokens, cotangent, gate_weight, up_weight, down_weight):
    gate = jnp.dot(tokens, gate_weight, preferred_element_type=jnp.float32)
    up = jnp.dot(tokens, up_weight, preferred_element_type=jnp.float32)
    sig = jax.nn.sigmoid(gate)
    act = gate * sig
    hidden = (act * up).astype(jnp.bfloat16)
    hidden_grad = lax.dot_general(cotangent, down_weight, (((1,), (0,)), ((), ())), preferred_element_type=jnp.float32)
    gate_cot = (hidden_grad * up * sig * (1.0 + gate * (1.0 - sig))).astype(jnp.bfloat16)
    up_cot = (hidden_grad * act).astype(jnp.bfloat16)
    width = FF // N_TP

    def add_block(total, index):
        start = (index * width).astype(jnp.int32)
        gate_part = lax.dynamic_slice_in_dim(gate_cot, start, width, 1)
        up_part = lax.dynamic_slice_in_dim(up_cot, start, width, 1)
        gate_rows = lax.dynamic_slice_in_dim(gate_weight, start, width, 1)
        up_rows = lax.dynamic_slice_in_dim(up_weight, start, width, 1)
        partial_value = lax.dot_general(gate_part, gate_rows, (((1,), (1,)), ((), ())), preferred_element_type=jnp.float32)
        partial_value = partial_value + lax.dot_general(up_part, up_rows, (((1,), (1,)), ((), ())), preferred_element_type=jnp.float32)
        rounded = lax.optimization_barrier(partial_value.astype(jnp.bfloat16))
        return total + rounded.astype(jnp.float32), None

    start_total = jnp.zeros((tokens.shape[0], tokens.shape[1]), jnp.float32)
    total, unused = lax.scan(add_block, start_total, jnp.arange(N_TP, dtype=jnp.int32))
    input_grad = total.astype(jnp.bfloat16)
    contract = (((0,), (0,)), ((), ()))
    gate_grad = lax.dot_general(tokens, gate_cot, contract, preferred_element_type=jnp.float32)
    up_grad = lax.dot_general(tokens, up_cot, contract, preferred_element_type=jnp.float32)
    down_grad = lax.dot_general(cotangent, hidden, contract, preferred_element_type=jnp.float32)
    return (input_grad, gate_grad, up_grad, down_grad)
```

```python
import jax
import jax.numpy as jnp
from jax import lax
from jax.sharding import PartitionSpec as P

CORES = 2
CHUNK = 176


def dot(left, right, left_dim, right_dim):
    return lax.dot_general(
        left, right, (((left_dim,), (right_dim,)), ((), ())), preferred_element_type=jnp.float32
    )


class Line:
    def __init__(self, chips):
        self.chips = chips

    def partner(self, z, even):
        step = 1 if (z % 2 == 0) == even else -1
        other = z + step
        return other if 0 <= other < self.chips else None

    def reach(self, z, even):
        return self.chips - 1 - z if (z % 2 == 0) == even else z

    def send(self, value, even, is_sender):
        pairs = [
            (z * CORES + core, self.partner(z, even) * CORES + core)
            for z in range(self.chips)
            if self.partner(z, even) is not None and is_sender(z)
            for core in range(CORES)
        ]
        return lax.ppermute(value, "fs", pairs) if pairs else None

    def gather(self, own):
        even, odd = [own], [own]
        for step in range(1, self.chips):
            new_even = self.send(odd[step - 1], True, lambda z: step - 1 <= self.reach(z, False))
            new_odd = self.send(even[step - 1], False, lambda z: step - 1 <= self.reach(z, True))
            even.append(new_even)
            odd.append(new_odd)
        return [own] + [plus(even[j], odd[self.chips - j]) for j in range(1, self.chips)]

    def reduce(self, slots):
        even, odd = None, None
        for step in range(self.chips - 1, 0, -1):
            to_even = rounded(plus(slots[step], odd))
            to_odd = rounded(plus(slots[self.chips - step], even))
            even = self.send(to_even, True, lambda z: step <= self.reach(z, True))
            odd = self.send(to_odd, False, lambda z: step <= self.reach(z, False))
        return plus(plus(slots[0].astype(jnp.float32), even), odd)


def plus(a, b):
    if a is None or b is None:
        return b if a is None else a
    if a.dtype == b.dtype == jnp.bfloat16:
        return a + b
    return a.astype(jnp.float32) + b.astype(jnp.float32)


def rounded(a):
    return a.astype(jnp.bfloat16)


def swap_cores(value):
    pairs = [(i, i ^ 1) for i in range(lax.axis_size("fs"))]
    return lax.ppermute(value, "fs", pairs)


def half_of(value, axis, index):
    width = value.shape[axis] // 2
    return lax.dynamic_slice_in_dim(value, index * width, width, axis)


def scatter_tp(value):
    size, rows, columns = lax.axis_size("tp"), value.shape[0], value.shape[1]
    bits = size.bit_length() - 1
    if size != 1 << bits:
        return lax.psum_scatter(value.astype(jnp.bfloat16), "tp", scatter_dimension=1, tiled=True)
    me = lax.axis_index("tp")
    width = columns // size
    parts = []
    blocks = value.reshape(rows, size, 2, width // 2)
    for half in range(2):
        held = blocks[:, :, half].reshape((rows,) + (2,) * bits + (width // 2,))
        order = range(bits) if half == 0 else range(bits - 1, -1, -1)
        left = list(range(bits))
        for bit in order:
            axis = 1 + (len(left) - 1 - left.index(bit))
            mine = (me >> bit) & 1
            keep = lax.dynamic_index_in_dim(held, mine, axis, keepdims=False)
            give = lax.dynamic_index_in_dim(held, 1 - mine, axis, keepdims=False)
            pairs = [(i, i ^ (1 << bit)) for i in range(size)]
            got = lax.ppermute(give.astype(jnp.bfloat16), "tp", pairs)
            held = keep.astype(jnp.float32) + got.astype(jnp.float32)
            left.remove(bit)
        parts.append(held.reshape(rows, width // 2))
    return jnp.concatenate([part.astype(jnp.bfloat16) for part in parts], axis=1)


def shards(tokens, cotangent, gate_weight, up_weight, down_weight):
    chips = lax.axis_size("fs") // CORES
    index = lax.axis_index("fs")
    chip, core = index // CORES, index % CORES
    line = Line(chips)
    rows, hidden_units = gate_weight.shape
    half = hidden_units // 2

    weights = jnp.stack([gate_weight.T, up_weight.T, down_weight.T])
    mine, other = half_of(weights, 1, core), half_of(weights, 1, 1 - core)
    own = jnp.concatenate([mine, swap_cores(other)], axis=2)
    both_tokens = jnp.concatenate([tokens, swap_cores(tokens)], axis=0)
    both_cotangent = jnp.concatenate([cotangent, swap_cores(cotangent)], axis=0)

    direction = 1 - 2 * (chip % 2)
    starts = []
    for slot in range(chips):
        where = (chip + direction * slot) % chips
        starts.append((where * CORES + core) * rows)
        starts.append((where * CORES + 1 - core) * rows)

    def reordered(value):
        return jnp.concatenate(
            [lax.dynamic_slice_in_dim(value, start, rows, 1) for start in starts], axis=1
        )

    token_blocks, cotangent_blocks = reordered(both_tokens), reordered(both_cotangent)

    width = CORES * rows
    chunks = max(1, half // CHUNK)
    cuts = [half * k // chunks // 16 * 16 for k in range(chunks)] + [half]
    input_terms = []
    sums = []
    for low, high in zip(cuts[:-1], cuts[1:]):
        size = high - low
        slots = line.gather(own[:, low:high].reshape(3 * size, width))
        whole = jnp.concatenate(slots, axis=1)
        gate_up = dot(whole[: 2 * size], token_blocks, 1, 1)
        gate, up = gate_up[:size], gate_up[size:]
        hidden_grad = dot(whole[2 * size :], cotangent_blocks, 1, 1)
        sig = jax.nn.sigmoid(gate)
        act = gate * sig
        hidden = rounded(act * up)
        gate_cot = rounded(hidden_grad * up * sig * (1.0 + gate * (1.0 - sig)))
        up_cot = rounded(hidden_grad * act)
        cots = jnp.concatenate([gate_cot, up_cot], axis=0)
        input_terms.append((cots, whole[: 2 * size]))
        grads = jnp.concatenate(
            [rounded(dot(cots, token_blocks, 1, 0)), rounded(dot(hidden, cotangent_blocks, 1, 0))], axis=0
        )
        total = line.reduce([grads[:, slot * width : (slot + 1) * width] for slot in range(chips)])
        sums.append(total.reshape(3, size, width))

    cots = jnp.concatenate([term[0] for term in input_terms], axis=0)
    whole = jnp.concatenate([term[1] for term in input_terms], axis=0)
    partial = rounded(dot(cots, whole, 0, 0))
    placed = jnp.zeros_like(partial)
    for position, start in enumerate(starts):
        placed = lax.dynamic_update_slice_in_dim(
            placed, partial[:, position * rows : (position + 1) * rows], start, 1
        )
    count = tokens.shape[0]
    chip_partial = placed[:count].astype(jnp.float32) + swap_cores(placed[count:]).astype(jnp.float32)
    input_grad = scatter_tp(chip_partial)

    total = jnp.concatenate(sums, axis=1)
    kept, given = total[:, :, :rows], swap_cores(total[:, :, rows:])
    halves = jnp.stack([kept, given])
    grads = jnp.concatenate(
        [
            lax.dynamic_index_in_dim(halves, core, 0, keepdims=False),
            lax.dynamic_index_in_dim(halves, 1 - core, 0, keepdims=False),
        ],
        axis=1,
    )
    return (input_grad, grads[0].T, grads[1].T, grads[2].T)


def solution(mesh):
    in_specs = (P("fs", None), P("fs", None), P("fs", "tp"), P("fs", "tp"), P("fs", "tp"))
    out_specs = (P("fs", "tp"), P("fs", "tp"), P("fs", "tp"), P("fs", "tp"))
    return jax.shard_map(shards, mesh=mesh, in_specs=in_specs, out_specs=out_specs, check_vma=False)
```

```python
import functools

import jax
import jax.numpy as jnp
from jax import lax
from jax.experimental import pallas as pl
from jax.experimental.pallas import tpu as pltpu
from jax.sharding import PartitionSpec as P


CORES = 2
CHUNK = 176
PARTS = (2, 2, 2)


def dot(left, right, left_dim, right_dim):
    return lax.dot_general(
        left, right, (((left_dim,), (right_dim,)), ((), ())), preferred_element_type=jnp.float32
    )


class Line:
    def __init__(self, chips):
        self.chips = chips
        index = lax.axis_index("fs")
        self.chip, self.core = index // CORES, index % CORES
        below = (self.chip % 2) == 0
        self.even_reach = jnp.where(below, chips - 1 - self.chip, self.chip)
        self.odd_reach = chips - 1 - self.even_reach

    def partner(self, z, even):
        other = z + (1 if (z % 2 == 0) == even else -1)
        return other if 0 <= other < self.chips else None

    def reach(self, z, even):
        return self.chips - 1 - z if (z % 2 == 0) == even else z

    def swap(self, value, even):
        pairs = []
        for z in range(self.chips):
            other = self.partner(z, even)
            for core in range(CORES):
                there = z * CORES + 1 - core if other is None else other * CORES + core
                pairs.append((z * CORES + core, there))
        return lax.ppermute(value, "fs", pairs)

    def stage(self, own, blocks):
        chips = self.chips
        parts = range(len(own if own is not None else blocks[0]))
        got = {True: [own], False: [own]}
        sums = {True: None, False: None}
        last = None
        for step in range(1, chips + 1):
            ahead = chips - step + 1
            new = {}
            for part in parts:
                for even in (True, False):
                    ends = [z for z in range(chips) if self.partner(z, even) is not None]
                    gathers = own is not None and step < chips and any(step - 1 <= self.reach(z, not even) for z in ends)
                    reduces = blocks is not None and step > 1 and any(ahead <= self.reach(z, even) for z in ends)
                    if not gathers and not reduces:
                        continue
                    if reduces:
                        block, other = blocks[ahead if even else chips - ahead][part], sums[not even]
                        if last is not None:
                            block, _ = lax.optimization_barrier((block, last))
                        value = rounded(plus(block, None if other is None else other[part]))
                    if gathers:
                        block = got[not even][step - 1][part]
                        behind = self.odd_reach if even else self.even_reach
                        value = jnp.where(behind >= step - 1, block, value) if reduces else block
                    last = value if reduces else last
                    moved = self.swap(value, even)
                    new.setdefault(even, []).append(moved)
            for even in (True, False):
                got[even].append(new.get(even))
                sums[even] = new.get(even) if step > 1 else None
            if sums[False] is not None:
                sums[False] = [jnp.where(self.odd_reach > 0, each, 0) for each in sums[False]]
        slots = total = None
        if own is not None:
            slots = [(own, None)] + [(got[True][j], got[False][chips - j]) for j in range(1, chips)]
        if blocks is not None:
            total = []
            for part in parts:
                value = blocks[0][part].astype(jnp.float32)
                for each in (sums[True], sums[False]):
                    value = value if each is None else plus(value, each[part])
                total.append(value)
            total = jnp.concatenate(total)
        return slots, total


def cut(value, parts):
    if parts == 1:
        return [value]
    middle = (value.shape[0] // 2 + 15) // 16 * 16
    return [value[:middle], value[middle:]]


def plus(a, b):
    if a is None or b is None:
        return b if a is None else a
    if a.dtype == b.dtype == jnp.bfloat16:
        return a + b
    return a.astype(jnp.float32) + b.astype(jnp.float32)


def rounded(a):
    return a.astype(jnp.bfloat16)


def swap_cores(value):
    pairs = [(i, i ^ 1) for i in range(lax.axis_size("fs"))]
    return lax.ppermute(value, "fs", pairs)


def split_kernel(orders, width, table, mine, theirs, *outs):
    for part, order in enumerate(orders):
        give, keep = outs[2 * part], outs[2 * part + 1]
        for out, place in ((give, 0), (keep, 1)):
            for i in range(len(order)):
                where = pl.ds(pl.multiple_of(table[(part * 2 + place) * len(order) + i] * width, width), width)
                both = mine[:, where].astype(jnp.float32) + theirs[:, where].astype(jnp.float32)
                out[:, i * width : (i + 1) * width] = both.astype(out.dtype)


def scatter_tp(mine, theirs):
    size, (rows, columns) = lax.axis_size("tp"), mine.shape
    bits = size.bit_length() - 1
    if size != 1 << bits or size == 1:
        return lax.psum_scatter(rounded(plus_wide(mine, theirs)), "tp", scatter_dimension=1, tiled=True)
    me = lax.axis_index("tp")
    width = columns // size // 2
    orders = [list(range(bits)), list(range(bits - 1, -1, -1))]
    rests = [[other for other in range(size) if not other >> order[0] & 1] for order in orders]
    table = []
    for part, (order, rest) in enumerate(zip(orders, rests)):
        table += [(me ^ (other | 1 << order[0])) * 2 + part for other in rest]
        table += [(me ^ other) * 2 + part for other in rest]
    if width % 128:
        both = plus_wide(mine, theirs)
        count = len(rests[0])
        split = []
        for i in range(4):
            picked = [lax.dynamic_slice_in_dim(both, table[i * count + j] * width, width, 1) for j in range(count)]
            split.append(jnp.concatenate(picked, 1).astype(jnp.float32 if i % 2 else jnp.bfloat16))
    else:
        out = [jax.ShapeDtypeStruct((rows, columns // 4), t) for t in (jnp.bfloat16, jnp.float32)] * 2
        split = pl.pallas_call(
            functools.partial(split_kernel, rests, width),
            out_shape=out,
            in_specs=[pl.BlockSpec(memory_space=pltpu.SMEM)] + [pl.BlockSpec(memory_space=pltpu.VMEM)] * 2,
            out_specs=[pl.BlockSpec(memory_space=pltpu.VMEM)] * 4,
            compiler_params=pltpu.CompilerParams(vmem_limit_bytes=20 * 1024 * 1024),
            cost_estimate=pl.CostEstimate(flops=rows * columns, bytes_accessed=8 * rows * columns, transcendentals=0),
        )(jnp.stack(table).astype(jnp.int32), mine, theirs)
    parts = []
    for part, (order, rest) in enumerate(zip(orders, rests)):
        give, keep = split[2 * part], split[2 * part + 1]
        for step, bit in enumerate(order):
            pairs = [(i, i ^ (1 << bit)) for i in range(size)]
            got = lax.ppermute(give, "tp", pairs)
            held = plus_wide(keep, got)
            if step + 1 < bits:
                left = [other for other in rest if not other >> order[step + 1] & 1]

                def pick(others):
                    spots = [rest.index(other) for other in others]
                    return jnp.concatenate([held[:, i * width : (i + 1) * width] for i in spots], 1)

                give, keep = rounded(pick([other | 1 << order[step + 1] for other in left])), pick(left)
                rest = left
        parts.append(rounded(held))
    return jnp.concatenate(parts, axis=1)


def plus_wide(a, b):
    return a.astype(jnp.float32) + b.astype(jnp.float32)


def input_kernel(chunks, *refs):
    cots, wholes, (mine, theirs) = refs[:chunks], refs[chunks : 2 * chunks], refs[2 * chunks :]
    for i, out in ((1, theirs), (0, mine)):
        value = None
        for cot, whole in zip(cots, wholes):
            value = plus(value, dot(cot[i], whole[...], 0, 0))
        out[...] = value.astype(out.dtype)


def input_terms(cots, wholes, rows):
    depth = wholes[0].shape[1]
    units = sum(cot.shape[1] for cot in cots)
    if depth % 128 or any(cot.shape[1] % 32 for cot in cots):
        whole = jnp.concatenate(wholes)
        return [rounded(dot(jnp.concatenate([cot[i] for cot in cots]), whole, 0, 0)) for i in range(CORES)]
    return pl.pallas_call(
        functools.partial(input_kernel, len(cots)),
        out_shape=[jax.ShapeDtypeStruct((rows, depth), jnp.bfloat16)] * 2,
        in_specs=[pl.BlockSpec(memory_space=pltpu.VMEM)] * (2 * len(cots)),
        out_specs=[pl.BlockSpec(memory_space=pltpu.VMEM)] * 2,
        compiler_params=pltpu.CompilerParams(vmem_limit_bytes=28 * 1024 * 1024),
        cost_estimate=pl.CostEstimate(
            flops=4 * rows * depth * units, bytes_accessed=2 * (units + 2 * rows) * depth, transcendentals=0
        ),
    )(*cots, *wholes)


def gated(gate, up, hidden_grad):
    sig = jax.nn.sigmoid(gate)
    act = gate * sig
    gate_cot = hidden_grad * up * sig * (1.0 + gate * (1.0 - sig))
    return rounded(act * up), rounded(gate_cot), rounded(hidden_grad * act)


def chunk_plain(places, slots, even_first, tokens, cotangents, size, parts):
    slots = [tuple(None if each is None else jnp.concatenate(each) for each in pair) for pair in slots]
    width = slots[0][0].shape[1]
    whole = jnp.zeros((3 * size, width * len(slots)), jnp.bfloat16)
    for place, (even, odd), flag in zip(places, slots, even_first):
        piece = odd if even is None else even if odd is None else jnp.where(flag == 0, even, odd)
        whole = lax.dynamic_update_slice_in_dim(whole, piece, place * width, 1)
    rows = tokens[0].shape[0]
    tokens, cotangents = jnp.concatenate(tokens), jnp.concatenate(cotangents)
    gate_up = dot(whole[: 2 * size], tokens, 1, 1)
    hidden_grad = dot(whole[2 * size :], cotangents, 1, 1)
    hidden, gate_cot, up_cot = gated(gate_up[:size], gate_up[size:], hidden_grad)
    cots = jnp.concatenate([gate_cot, up_cot])
    grads = jnp.concatenate([dot(cots, tokens, 1, 0), dot(hidden, cotangents, 1, 0)])
    blocks = [lax.dynamic_slice_in_dim(grads, place * width, width, 1) for place in places]
    cots = cots.reshape(2 * size, CORES, rows).swapaxes(0, 1)
    return [cut(rounded(block), parts) for block in blocks], cots, whole[: 2 * size]


def chunk_kernel(layout, cuts_in, cuts_out, size, held, width, *refs):
    chips, parts_in, parts_out = len(layout), len(cuts_in) - 1, len(cuts_out) - 1
    count = sum(len(sources) for sources in layout) * parts_in
    table, pieces, refs = refs[0], refs[1 : 1 + count], refs[1 + count :]
    inputs, refs = refs[:held], refs[held:]
    count = chips * parts_out
    blocks_out, cots_out, whole_out = refs[:count], refs[count], refs[count + 1]
    whole, blocks, cots, hidden, piece_sem, out_sem, cots_sem = refs[count + 2 : count + 9]
    if held == 2:
        tokens, cotangents = inputs
    else:
        tokens, cotangents, input_sem = refs[count + 9 :]

    def stage_in(i):
        return [
            pltpu.make_async_copy(inputs[i], tokens.at[i], input_sem.at[0, i]),
            pltpu.make_async_copy(inputs[CORES + i], cotangents.at[i], input_sem.at[1, i]),
        ]

    def columns(slot):
        return pl.ds(pl.multiple_of(table[slot] * width, width), width)

    def loads(position, slot):
        return [
            pltpu.make_async_copy(
                pieces[position * parts_in + part],
                whole.at[cuts_in[part] : cuts_in[part + 1], columns(slot)],
                piece_sem.at[slot * parts_in + part],
            )
            for part in range(parts_in)
        ]

    position = 0
    for slot, sources in enumerate(layout):
        for source in sources:
            if len(sources) == 1:
                for load in loads(position, slot):
                    load.start()
            else:

                @pl.when(table[chips + slot] == source)
                def _():
                    for load in loads(position, slot):
                        load.start()

            position += 1
    if held != 2:
        for i in range(CORES):
            for copy in stage_in(i):
                copy.start()
    position = 0
    for slot, sources in enumerate(layout):
        for load in loads(position, slot):
            load.wait()
        position += len(sources)
    outs = [pltpu.make_async_copy(whole.at[: 2 * size], whole_out, cots_sem.at[CORES])]
    outs[0].start()

    if held != 2:
        for i in range(CORES):
            for copy in stage_in(i):
                copy.wait()

    def forward(i, carry):
        gate_up = dot(whole[: 2 * size], tokens[i], 1, 1)
        hidden_grad = dot(whole[2 * size :], cotangents[i], 1, 1)
        hidden[i], cots[i, :size], cots[i, size:] = gated(gate_up[:size], gate_up[size:], hidden_grad)
        return carry

    lax.fori_loop(0, CORES, forward, 0)
    for i in range(CORES):
        outs.append(pltpu.make_async_copy(cots.at[i], cots_out.at[i], cots_sem.at[i]))
        outs[-1].start()

    def stores(slot):
        return [
            pltpu.make_async_copy(
                blocks.at[slot, cuts_out[part] : cuts_out[part + 1]],
                blocks_out[slot * parts_out + part],
                out_sem.at[slot * parts_out + part],
            )
            for part in range(parts_out)
        ]

    def gradient(step, carry):
        slot = chips - 1 - step
        where = columns(slot)
        value = dot(cots[0], tokens[0, :, where], 1, 0) + dot(cots[1], tokens[1, :, where], 1, 0)
        blocks[slot, : 2 * size] = value.astype(blocks.dtype)
        value = dot(hidden[0], cotangents[0, :, where], 1, 0) + dot(hidden[1], cotangents[1, :, where], 1, 0)
        blocks[slot, 2 * size :] = value.astype(blocks.dtype)
        for each in range(chips):

            @pl.when(slot == each)
            def _():
                for store in stores(each):
                    store.start()

        return carry

    lax.fori_loop(0, chips, gradient, 0)
    for slot in range(chips):
        outs += stores(slot)
    for copy in outs:
        copy.wait()


def in_hbm(value):
    return pltpu.with_memory_space_constraint(value, pltpu.MemorySpace.HBM)


def in_vmem(value):
    return pltpu.with_memory_space_constraint(value, pltpu.VMEM)


def chunk_fused(places, slots, even_first, tokens, cotangents, size, parts):
    chips, width = len(slots), slots[0][0][0].shape[1]
    inputs = [in_hbm(each) for each in (*tokens, *cotangents)] if isinstance(tokens, list) else [tokens, cotangents]
    rows, depth = tokens[0].shape
    held = len(inputs)
    if held == 2:
        inputs = [in_vmem(each) for each in inputs]
    layout = [tuple(i for i in range(2) if pair[i] is not None) for pair in slots]
    pieces = [in_hbm(each) for pair, sources in zip(slots, layout) for i in sources for each in pair[i]]
    table = jnp.stack([jnp.asarray(v, jnp.int32) for v in places + even_first])
    hbm = pltpu.MemorySpace.HBM
    free = hbm
    block = (3 * size, width)

    def cuts(shapes):
        ends = [0]
        for shape in shapes:
            ends.append(ends[-1] + shape[0])
        return ends

    shapes = [each.shape for each in cut(jax.ShapeDtypeStruct(block, jnp.bfloat16), 1)]
    if parts == 2:
        middle = (block[0] // 2 + 15) // 16 * 16
        shapes = [(middle, width), (block[0] - middle, width)]
    cuts_in, cuts_out = cuts([each.shape for each in slots[0][0]]), cuts(shapes)
    flops = 2 * 2 * 3 * size * depth * 2 * rows
    out = pl.pallas_call(
        functools.partial(chunk_kernel, layout, cuts_in, cuts_out, size, held, width),
        out_shape=[hbm(shape, jnp.bfloat16) for _ in range(chips) for shape in shapes]
        + [free((CORES, 2 * size, rows), jnp.bfloat16), free((2 * size, depth), jnp.bfloat16)],
        in_specs=[pl.BlockSpec(memory_space=pltpu.SMEM)]
        + [pl.BlockSpec(memory_space=hbm)] * len(pieces)
        + [pl.BlockSpec(memory_space=pltpu.VMEM if held == 2 else hbm)] * held,
        out_specs=[pl.BlockSpec(memory_space=pl.ANY)] * (chips * parts + 2),
        scratch_shapes=[
            pltpu.VMEM((3 * size, depth), jnp.bfloat16),
            pltpu.VMEM((chips,) + block, jnp.bfloat16),
            pltpu.VMEM((CORES, 2 * size, rows), jnp.bfloat16),
            pltpu.VMEM((CORES, size, rows), jnp.bfloat16),
            pltpu.SemaphoreType.DMA((chips * (len(cuts_in) - 1),)),
            pltpu.SemaphoreType.DMA((chips * parts,)),
            pltpu.SemaphoreType.DMA((CORES + 1,)),
        ]
        + ([pltpu.VMEM((CORES, rows, depth), jnp.bfloat16)] * 2 + [pltpu.SemaphoreType.DMA((2, CORES))]) * (held != 2),
        compiler_params=pltpu.CompilerParams(vmem_limit_bytes=(24 if held == 2 else 32) * 1024 * 1024),
        cost_estimate=pl.CostEstimate(flops=flops, bytes_accessed=16 * size * depth, transcendentals=size * rows * 2),
    )(table, *pieces, *inputs)
    return [out[slot * parts : (slot + 1) * parts] for slot in range(chips)], out[-2], out[-1]


def layer(tokens, cotangent, gate_weight, up_weight, down_weight):
    chips = lax.axis_size("fs") // CORES
    index = lax.axis_index("fs")
    chip, core = index // CORES, index % CORES
    line = Line(chips)
    rows, hidden_units = gate_weight.shape
    half = hidden_units // 2
    width = CORES * rows

    direction = 1 - 2 * (chip % 2)
    places = [(chip + direction * slot) % chips for slot in range(chips)]
    reach = jnp.where(chip % 2 == 0, chips - 1 - chip, chip)
    even_first = [jnp.where(slot <= reach, 0, 1) for slot in range(chips)]

    weights = [gate_weight.T, up_weight.T, down_weight.T]

    def rows_of(arrays, start, size):
        return jnp.concatenate([lax.dynamic_slice_in_dim(w, start, size, 0) for w in arrays])

    chunks = max(1, half // CHUNK)
    cuts = [half * k // chunks // 16 * 16 for k in range(chunks)] + [half]
    owns = []

    def own_block(k, weights):
        low, high = cuts[k], cuts[k + 1]
        mine, other = rows_of(weights, core * half + low, high - low), rows_of(weights, (1 - core) * half + low, high - low)
        other = swap_cores(other)
        return jnp.where(core == 0, jnp.concatenate([mine, other], 1), jnp.concatenate([other, mine], 1))

    owns.append(own_block(0, weights))
    tokens, cotangent, _ = lax.optimization_barrier((tokens, cotangent, owns[0]))
    tokens = [tokens, swap_cores(tokens)]
    cotangents = [cotangent, swap_cores(cotangent)]
    count = cotangent.shape[0]

    terms = []
    kept, given = [], []
    blocks = None
    for k in range(chunks + 1):
        if 0 < k < chunks:
            *later, _ = lax.optimization_barrier((*weights, slots[1][0][0]))
            owns.append(own_block(k, later))
        own = cut(owns[k], PARTS[k % len(PARTS)]) if k < chunks else None
        slots, total = line.stage(own, blocks)
        if total is not None:
            kept.append(lax.dynamic_slice_in_dim(total, core * rows, rows, 1))
            given.append(swap_cores(lax.dynamic_slice_in_dim(total, (1 - core) * rows, rows, 1)))
        if slots is not None:
            size = cuts[k + 1] - cuts[k]
            parts = PARTS[(k + 1) % len(PARTS)]
            if width % 128 or size % 16:
                blocks, cots, whole = chunk_plain(places, slots, even_first, tokens, cotangents, size, parts)
            else:
                if k > 0:
                    values, _ = lax.optimization_barrier(((tokens, cotangents), blocks[0][0]))
                    values = [jnp.stack(value) for value in values]
                else:
                    values = (tokens, cotangents)
                blocks, cots, whole = chunk_fused(places, slots, even_first, *values, size, parts)
            terms.append((cots, whole))

    mine, theirs = input_terms([term[0] for term in terms], [term[1] for term in terms], count)
    input_grad = scatter_tp(mine, swap_cores(theirs))

    grads = []
    for i in range(3):

        def column(parts):
            return [part.reshape(3, -1, rows)[i] for part in parts]

        first = jnp.concatenate(column(kept) + column(given))
        second = jnp.concatenate(column(given) + column(kept))
        grads.append(jnp.where(core == 0, first, second).T)
    return (input_grad, *grads)


def solution(mesh):
    in_specs = (P("fs", None), P("fs", None), P("fs", "tp"), P("fs", "tp"), P("fs", "tp"))
    out_specs = (P("fs", "tp"), P("fs", "tp"), P("fs", "tp"), P("fs", "tp"))
    return jax.shard_map(layer, mesh=mesh, in_specs=in_specs, out_specs=out_specs, check_vma=False)
```

```python
import functools

import jax
import jax.numpy as jnp
from jax import lax
from jax.experimental import pallas as pl
from jax.experimental.pallas import tpu as pltpu
from jax.sharding import PartitionSpec as P


CORES = 2
CHUNK = 176
FIRST = (2, 3)
PARTS = (2, 2, 2)


def dot(left, right, left_dim, right_dim):
    return lax.dot_general(
        left, right, (((left_dim,), (right_dim,)), ((), ())), preferred_element_type=jnp.float32
    )


class Line:
    def __init__(self, chips):
        self.chips = chips
        index = lax.axis_index("fs")
        self.chip, self.core = index // CORES, index % CORES
        below = (self.chip % 2) == 0
        self.even_reach = jnp.where(below, chips - 1 - self.chip, self.chip)
        self.odd_reach = chips - 1 - self.even_reach

    def partner(self, z, even):
        other = z + (1 if (z % 2 == 0) == even else -1)
        return other if 0 <= other < self.chips else None

    def reach(self, z, even):
        return self.chips - 1 - z if (z % 2 == 0) == even else z

    def swap(self, value, even):
        pairs = []
        for z in range(self.chips):
            other = self.partner(z, even)
            for core in range(CORES):
                there = z * CORES + 1 - core if other is None else other * CORES + core
                pairs.append((z * CORES + core, there))
        return lax.ppermute(value, "fs", pairs)

    def stage(self, own, blocks):
        chips = self.chips
        parts = range(len(own if own is not None else blocks[0]))
        got = {True: [own], False: [own]}
        sums = {True: None, False: None}
        last = None
        for step in range(1, chips + 1):
            ahead = chips - step + 1
            new = {}
            for part in parts:
                for even in (True, False):
                    ends = [z for z in range(chips) if self.partner(z, even) is not None]
                    gathers = own is not None and step < chips and any(step - 1 <= self.reach(z, not even) for z in ends)
                    reduces = blocks is not None and step > 1 and any(ahead <= self.reach(z, even) for z in ends)
                    if not gathers and not reduces:
                        continue
                    if reduces:
                        block, other = blocks[ahead if even else chips - ahead][part], sums[not even]
                        if last is not None:
                            block, _ = lax.optimization_barrier((block, last))
                        value = rounded(plus(block, None if other is None else other[part]))
                    if gathers:
                        block = got[not even][step - 1][part]
                        behind = self.odd_reach if even else self.even_reach
                        value = jnp.where(behind >= step - 1, block, value) if reduces else block
                    last = value if reduces else last
                    moved = self.swap(value, even)
                    new.setdefault(even, []).append(moved)
            for even in (True, False):
                got[even].append(new.get(even))
                sums[even] = new.get(even) if step > 1 else None
            if sums[False] is not None:
                sums[False] = [jnp.where(self.odd_reach > 0, each, 0) for each in sums[False]]
        slots = total = None
        if own is not None:
            slots = [(own, None)] + [(got[True][j], got[False][chips - j]) for j in range(1, chips)]
        if blocks is not None:
            total = []
            for part in parts:
                value = blocks[0][part].astype(jnp.float32)
                for each in (sums[True], sums[False]):
                    value = value if each is None else plus(value, each[part])
                total.append(value)
            total = jnp.concatenate(total)
        return slots, total


def cut(value, parts):
    if parts == 1:
        return [value]
    middle = (value.shape[0] // 2 + 15) // 16 * 16
    return [value[:middle], value[middle:]]


def plus(a, b):
    if a is None or b is None:
        return b if a is None else a
    if a.dtype == b.dtype == jnp.bfloat16:
        return a + b
    return a.astype(jnp.float32) + b.astype(jnp.float32)


def rounded(a):
    return a.astype(jnp.bfloat16)


def swap_cores(value):
    pairs = [(i, i ^ 1) for i in range(lax.axis_size("fs"))]
    return lax.ppermute(value, "fs", pairs)


def split_kernel(orders, width, table, mine, theirs, *outs):
    for part, order in enumerate(orders):
        give, keep = outs[2 * part], outs[2 * part + 1]
        for out, place in ((give, 0), (keep, 1)):
            for i in range(len(order)):
                where = pl.ds(pl.multiple_of(table[(part * 2 + place) * len(order) + i] * width, width), width)
                both = mine[:, where].astype(jnp.float32) + theirs[:, where].astype(jnp.float32)
                out[:, i * width : (i + 1) * width] = both.astype(out.dtype)


def scatter_tp(mine, theirs):
    size, (rows, columns) = lax.axis_size("tp"), mine.shape
    bits = size.bit_length() - 1
    if size != 1 << bits or size == 1:
        return lax.psum_scatter(rounded(plus_wide(mine, theirs)), "tp", scatter_dimension=1, tiled=True)
    me = lax.axis_index("tp")
    width = columns // size // 2
    orders = [list(range(bits)), list(range(bits - 1, -1, -1))]
    rests = [[other for other in range(size) if not other >> order[0] & 1] for order in orders]
    table = []
    for part, (order, rest) in enumerate(zip(orders, rests)):
        table += [(me ^ (other | 1 << order[0])) * 2 + part for other in rest]
        table += [(me ^ other) * 2 + part for other in rest]
    if width % 128:
        both = plus_wide(mine, theirs)
        count = len(rests[0])
        split = []
        for i in range(4):
            picked = [lax.dynamic_slice_in_dim(both, table[i * count + j] * width, width, 1) for j in range(count)]
            split.append(jnp.concatenate(picked, 1).astype(jnp.float32 if i % 2 else jnp.bfloat16))
    else:
        out = [jax.ShapeDtypeStruct((rows, columns // 4), t) for t in (jnp.bfloat16, jnp.float32)] * 2
        split = pl.pallas_call(
            functools.partial(split_kernel, rests, width),
            out_shape=out,
            in_specs=[pl.BlockSpec(memory_space=pltpu.SMEM)] + [pl.BlockSpec(memory_space=pltpu.VMEM)] * 2,
            out_specs=[pl.BlockSpec(memory_space=pltpu.VMEM)] * 4,
            compiler_params=pltpu.CompilerParams(vmem_limit_bytes=20 * 1024 * 1024),
            cost_estimate=pl.CostEstimate(flops=rows * columns, bytes_accessed=8 * rows * columns, transcendentals=0),
        )(jnp.stack(table).astype(jnp.int32), mine, theirs)
    parts = []
    for part, (order, rest) in enumerate(zip(orders, rests)):
        give, keep = split[2 * part], split[2 * part + 1]
        for step, bit in enumerate(order):
            pairs = [(i, i ^ (1 << bit)) for i in range(size)]
            got = lax.ppermute(give, "tp", pairs)
            held = plus_wide(keep, got)
            if step + 1 < bits:
                left = [other for other in rest if not other >> order[step + 1] & 1]

                def pick(others):
                    spots = [rest.index(other) for other in others]
                    return jnp.concatenate([held[:, i * width : (i + 1) * width] for i in spots], 1)

                give, keep = rounded(pick([other | 1 << order[step + 1] for other in left])), pick(left)
                rest = left
        parts.append(rounded(held))
    return jnp.concatenate(parts, axis=1)


def plus_wide(a, b):
    return a.astype(jnp.float32) + b.astype(jnp.float32)


def input_kernel(chunks, *refs):
    cots, wholes, (mine, theirs) = refs[:chunks], refs[chunks : 2 * chunks], refs[2 * chunks :]
    for i, out in ((1, theirs), (0, mine)):
        value = None
        for cot, whole in zip(cots, wholes):
            value = plus(value, dot(cot[i], whole[...], 0, 0))
        out[...] = value.astype(out.dtype)


def input_terms(cots, wholes, rows):
    depth = wholes[0].shape[1]
    units = sum(cot.shape[1] for cot in cots)
    if depth % 128 or any(cot.shape[1] % 32 for cot in cots):
        whole = jnp.concatenate(wholes)
        return [rounded(dot(jnp.concatenate([cot[i] for cot in cots]), whole, 0, 0)) for i in range(CORES)]
    return pl.pallas_call(
        functools.partial(input_kernel, len(cots)),
        out_shape=[jax.ShapeDtypeStruct((rows, depth), jnp.bfloat16)] * 2,
        in_specs=[pl.BlockSpec(memory_space=pltpu.VMEM)] * (2 * len(cots)),
        out_specs=[pl.BlockSpec(memory_space=pltpu.VMEM)] * 2,
        compiler_params=pltpu.CompilerParams(vmem_limit_bytes=28 * 1024 * 1024),
        cost_estimate=pl.CostEstimate(
            flops=4 * rows * depth * units, bytes_accessed=2 * (units + 2 * rows) * depth, transcendentals=0
        ),
    )(*cots, *wholes)


def gated(gate, up, hidden_grad):
    sig = jax.nn.sigmoid(gate)
    act = gate * sig
    gate_cot = hidden_grad * up * sig * (1.0 + gate * (1.0 - sig))
    return rounded(act * up), rounded(gate_cot), rounded(hidden_grad * act)


def chunk_plain(places, slots, even_first, tokens, cotangents, size, parts):
    slots = [tuple(None if each is None else jnp.concatenate(each) for each in pair) for pair in slots]
    width = slots[0][0].shape[1]
    whole = jnp.zeros((3 * size, width * len(slots)), jnp.bfloat16)
    for place, (even, odd), flag in zip(places, slots, even_first):
        piece = odd if even is None else even if odd is None else jnp.where(flag == 0, even, odd)
        whole = lax.dynamic_update_slice_in_dim(whole, piece, place * width, 1)
    rows = tokens[0].shape[0]
    tokens, cotangents = jnp.concatenate(tokens), jnp.concatenate(cotangents)
    gate_up = dot(whole[: 2 * size], tokens, 1, 1)
    hidden_grad = dot(whole[2 * size :], cotangents, 1, 1)
    hidden, gate_cot, up_cot = gated(gate_up[:size], gate_up[size:], hidden_grad)
    cots = jnp.concatenate([gate_cot, up_cot])
    grads = jnp.concatenate([dot(cots, tokens, 1, 0), dot(hidden, cotangents, 1, 0)])
    blocks = [lax.dynamic_slice_in_dim(grads, place * width, width, 1) for place in places]
    cots = cots.reshape(2 * size, CORES, rows).swapaxes(0, 1)
    return [cut(rounded(block), parts) for block in blocks], cots, whole[: 2 * size]


def chunk_kernel(layout, cuts_in, cuts_out, size, first, width, *refs):
    chips, parts_in, parts_out = len(layout), len(cuts_in) - 1, len(cuts_out) - 1
    count = sum(len(sources) for sources in layout) * parts_in
    table, pieces, refs = refs[0], refs[1 : 1 + count], refs[1 + count :]
    inputs, refs = refs[:2], refs[2:]
    count = first * parts_out
    blocks_out, cots_out, hidden_out, whole_out = refs[:count], refs[count], refs[count + 1], refs[count + 2]
    whole, blocks, cots, hidden, piece_sem, out_sem, cots_sem = refs[count + 3 :]
    tokens, cotangents = inputs

    def columns(slot):
        return pl.ds(pl.multiple_of(table[slot] * width, width), width)

    def loads(position, slot):
        return [
            pltpu.make_async_copy(
                pieces[position * parts_in + part],
                whole.at[cuts_in[part] : cuts_in[part + 1], columns(slot)],
                piece_sem.at[slot * parts_in + part],
            )
            for part in range(parts_in)
        ]

    position = 0
    for slot, sources in enumerate(layout):
        for source in sources:
            if len(sources) == 1:
                for load in loads(position, slot):
                    load.start()
            else:

                @pl.when(table[chips + slot] == source)
                def _():
                    for load in loads(position, slot):
                        load.start()

            position += 1
    position = 0
    for slot, sources in enumerate(layout):
        for load in loads(position, slot):
            load.wait()
        position += len(sources)
    outs = [pltpu.make_async_copy(whole.at[: 2 * size], whole_out, cots_sem.at[2 * CORES])]
    outs[0].start()

    def forward(i, carry):
        gate_up = dot(whole[: 2 * size], tokens[i], 1, 1)
        hidden_grad = dot(whole[2 * size :], cotangents[i], 1, 1)
        hidden[i], cots[i, :size], cots[i, size:] = gated(gate_up[:size], gate_up[size:], hidden_grad)
        return carry

    lax.fori_loop(0, CORES, forward, 0)
    for i in range(CORES):
        outs.append(pltpu.make_async_copy(cots.at[i], cots_out.at[i], cots_sem.at[i]))
        outs.append(pltpu.make_async_copy(hidden.at[i], hidden_out.at[i], cots_sem.at[CORES + i]))
        outs[-2].start()
        outs[-1].start()
    slots = range(chips - 1, chips - 1 - first, -1)

    def columns_of(value, core, i):
        return value[core, :, columns(slots[0] - i)]

    outs += gradients(slots, size, cots, hidden, tokens, cotangents, columns_of, blocks, blocks_out, cuts_out, out_sem)
    for copy in outs:
        copy.wait()


def gradients(slots, size, cots, hidden, tokens, cotangents, columns_of, blocks, blocks_out, cuts_out, sem):
    parts = len(cuts_out) - 1

    def stores(i):
        return [
            pltpu.make_async_copy(
                blocks.at[i, cuts_out[part] : cuts_out[part + 1]], blocks_out[i * parts + part], sem.at[i * parts + part]
            )
            for part in range(parts)
        ]

    def gradient(i, carry):
        for rows, left, right in ((slice(0, 2 * size), cots, tokens), (slice(2 * size, 3 * size), hidden, cotangents)):
            value = dot(left[0], columns_of(right, 0, i), 1, 0) + dot(left[1], columns_of(right, 1, i), 1, 0)
            blocks[i, rows] = value.astype(blocks.dtype)
        for each in range(len(slots)):

            @pl.when(i == each)
            def _():
                for store in stores(each):
                    store.start()

        return carry

    lax.fori_loop(0, len(slots), gradient, 0)
    return [store for i in range(len(slots)) for store in stores(i)]


def rest_kernel(slots, cuts_out, size, width, table, cots, hidden, *refs):
    inputs, refs = refs[: 2 * CORES], refs[2 * CORES :]
    blocks_out, (tokens, cotangents, blocks, load_sem, sem) = refs[:-5], refs[-5:]
    loads = []
    for i, slot in enumerate(slots):
        where = pl.ds(pl.multiple_of(table[slot] * width, width), width)
        for j, each in enumerate(inputs):
            held = (tokens, cotangents)[j // CORES].at[i, j % CORES]
            loads.append(pltpu.make_async_copy(each.at[:, where], held, load_sem.at[i, j]))
            loads[-1].start()
    for load in loads:
        load.wait()

    def columns_of(value, core, i):
        return value[i, core]

    outs = gradients(slots, size, cots, hidden, tokens, cotangents, columns_of, blocks, blocks_out, cuts_out, sem)
    for copy in outs:
        copy.wait()


def in_hbm(value):
    return pltpu.with_memory_space_constraint(value, pltpu.MemorySpace.HBM)


def in_vmem(value):
    return pltpu.with_memory_space_constraint(value, pltpu.VMEM)


def chunk_fused(first, places, slots, even_first, tokens, cotangents, apart, size, parts):
    chips, width = len(slots), slots[0][0][0].shape[1]
    rows, depth = tokens.shape[1:]
    layout = [tuple(i for i in range(2) if pair[i] is not None) for pair in slots]
    pieces = [in_hbm(each) for pair, sources in zip(slots, layout) for i in sources for each in pair[i]]
    table = jnp.stack([jnp.asarray(v, jnp.int32) for v in places + even_first])
    hbm = pltpu.MemorySpace.HBM
    block = (3 * size, width)
    middle = (block[0] // 2 + 15) // 16 * 16
    cuts_out = [0, middle, block[0]] if parts == 2 else [0, block[0]]
    cuts_in = [0]
    for each in slots[0][0]:
        cuts_in.append(cuts_in[-1] + each.shape[0])
    flops = 2 * 3 * size * depth * 2 * rows
    shapes = [hbm((high - low, width), jnp.bfloat16) for low, high in zip(cuts_out[:-1], cuts_out[1:])]
    smem, vmem = pl.BlockSpec(memory_space=pltpu.SMEM), pl.BlockSpec(memory_space=pltpu.VMEM)
    anywhere = pl.BlockSpec(memory_space=pl.ANY)
    tokens, cotangents = in_vmem(tokens), in_vmem(cotangents)
    out = pl.pallas_call(
        functools.partial(chunk_kernel, layout, cuts_in, cuts_out, size, first, width),
        out_shape=shapes * first
        + [
            hbm((CORES, 2 * size, rows), jnp.bfloat16),
            hbm((CORES, size, rows), jnp.bfloat16),
            hbm((2 * size, depth), jnp.bfloat16),
        ],
        in_specs=[smem] + [pl.BlockSpec(memory_space=hbm)] * len(pieces) + [vmem] * 2,
        out_specs=[anywhere] * (first * parts + 3),
        scratch_shapes=[
            pltpu.VMEM((3 * size, depth), jnp.bfloat16),
            pltpu.VMEM((first,) + block, jnp.bfloat16),
            pltpu.VMEM((CORES, 2 * size, rows), jnp.bfloat16),
            pltpu.VMEM((CORES, size, rows), jnp.bfloat16),
            pltpu.SemaphoreType.DMA((chips * (len(cuts_in) - 1),)),
            pltpu.SemaphoreType.DMA((first * parts,)),
            pltpu.SemaphoreType.DMA((2 * CORES + 1,)),
        ],
        compiler_params=pltpu.CompilerParams(vmem_limit_bytes=24 * 1024 * 1024),
        cost_estimate=pl.CostEstimate(
            flops=2 * flops, bytes_accessed=16 * size * depth, transcendentals=size * rows * 2
        ),
    )(table, *pieces, tokens, cotangents)
    firsts, (cots, hidden, whole) = out[: first * parts], out[first * parts :]
    left = range(chips - 1 - first, -1, -1)
    rests = pl.pallas_call(
        functools.partial(rest_kernel, left, cuts_out, size, width),
        out_shape=shapes * len(left),
        in_specs=[smem] + [vmem] * 2 + [pl.BlockSpec(memory_space=hbm)] * len(apart),
        out_specs=[anywhere] * (len(left) * parts),
        scratch_shapes=[
            pltpu.VMEM((len(left), CORES, rows, width), jnp.bfloat16),
            pltpu.VMEM((len(left), CORES, rows, width), jnp.bfloat16),
            pltpu.VMEM((len(left),) + block, jnp.bfloat16),
            pltpu.SemaphoreType.DMA((len(left), len(apart))),
            pltpu.SemaphoreType.DMA((len(left) * parts,)),
        ],
        compiler_params=pltpu.CompilerParams(vmem_limit_bytes=20 * 1024 * 1024),
        cost_estimate=pl.CostEstimate(flops=flops, bytes_accessed=8 * size * depth, transcendentals=0),
    )(table, cots, hidden, *[in_hbm(each) for each in apart])
    flat = list(firsts) + list(rests)
    blocks = [flat[i * parts : (i + 1) * parts] for i in range(chips - 1, -1, -1)]
    return blocks, cots, whole


def layer(tokens, cotangent, gate_weight, up_weight, down_weight):
    chips = lax.axis_size("fs") // CORES
    index = lax.axis_index("fs")
    chip, core = index // CORES, index % CORES
    line = Line(chips)
    rows, hidden_units = gate_weight.shape
    half = hidden_units // 2
    width = CORES * rows

    direction = 1 - 2 * (chip % 2)
    places = [(chip + direction * slot) % chips for slot in range(chips)]
    reach = jnp.where(chip % 2 == 0, chips - 1 - chip, chip)
    even_first = [jnp.where(slot <= reach, 0, 1) for slot in range(chips)]

    weights = [gate_weight.T, up_weight.T, down_weight.T]

    def rows_of(arrays, start, size):
        return jnp.concatenate([lax.dynamic_slice_in_dim(w, start, size, 0) for w in arrays])

    chunks = max(1, half // CHUNK)
    cuts = [half * k // chunks // 16 * 16 for k in range(chunks)] + [half]
    owns = []

    def own_block(k, weights):
        low, high = cuts[k], cuts[k + 1]
        mine, other = rows_of(weights, core * half + low, high - low), rows_of(weights, (1 - core) * half + low, high - low)
        other = swap_cores(other)
        return jnp.where(core == 0, jnp.concatenate([mine, other], 1), jnp.concatenate([other, mine], 1))

    owns.append(own_block(0, weights))
    tokens, cotangent, _ = lax.optimization_barrier((tokens, cotangent, owns[0]))
    tokens = [tokens, swap_cores(tokens)]
    cotangents = [cotangent, swap_cores(cotangent)]
    count = cotangent.shape[0]

    terms = []
    kept, given = [], []
    blocks = None
    for k in range(chunks + 1):
        if 0 < k < chunks:
            *later, _ = lax.optimization_barrier((*weights, slots[1][0][0]))
            owns.append(own_block(k, later))
        own = cut(owns[k], PARTS[k % len(PARTS)]) if k < chunks else None
        slots, total = line.stage(own, blocks)
        if total is not None:
            kept.append(lax.dynamic_slice_in_dim(total, core * rows, rows, 1))
            given.append(swap_cores(lax.dynamic_slice_in_dim(total, (1 - core) * rows, rows, 1)))
        if slots is not None:
            size = cuts[k + 1] - cuts[k]
            parts = PARTS[(k + 1) % len(PARTS)]
            if width % 128 or size % 16 or chips <= max(FIRST):
                blocks, cots, whole = chunk_plain(places, slots, even_first, tokens, cotangents, size, parts)
            else:
                after = slots[1][0][0] if k == 0 else blocks[0][0]
                values, _ = lax.optimization_barrier(((tokens, cotangents), after))
                values = [jnp.stack(value) for value in values]
                blocks, cots, whole = chunk_fused(
                    FIRST[k == chunks - 1], places, slots, even_first, *values, tokens + cotangents, size, parts
                )
            terms.append((cots, whole))

    mine, theirs = input_terms([term[0] for term in terms], [term[1] for term in terms], count)
    input_grad = scatter_tp(mine, swap_cores(theirs))

    grads = []
    for i in range(3):

        def column(parts):
            return [part.reshape(3, -1, rows)[i] for part in parts]

        first = jnp.concatenate(column(kept) + column(given))
        second = jnp.concatenate(column(given) + column(kept))
        grads.append(jnp.where(core == 0, first, second).T)
    return (input_grad, *grads)


def solution(mesh):
    in_specs = (P("fs", None), P("fs", None), P("fs", "tp"), P("fs", "tp"), P("fs", "tp"))
    out_specs = (P("fs", "tp"), P("fs", "tp"), P("fs", "tp"), P("fs", "tp"))
    return jax.shard_map(layer, mesh=mesh, in_specs=in_specs, out_specs=out_specs, check_vma=False)
```
